32 devices in a mesh: sp: 8 (over z, y), tp: 4 (over x, core).
Axes of the slice: x: 2, y: 2, z: 4, core: 2. Of those that a mesh axis runs over, the one named last changes fastest.
Arguments:
- target: bfloat16 [2048, 2048], P(('sp', 'tp')), may hold values from -6 to 6
- source: bfloat16 [4096, 2048], P(('sp', 'tp')), may hold values from -6 to 6
- target_gain: bfloat16 [2, 2048], replicated, may hold values from 0.099609375 to 1.8984375
- source_gain: bfloat16 [2, 2048], replicated, may hold values from 0.099609375 to 1.8984375
- query_w: bfloat16 [2, 2048, 8192], P(None, None, 'tp'), may hold values from -0.125 to 0.125
- key_w: bfloat16 [2, 2048, 4096], P(None, None, 'tp'), may hold values from -0.125 to 0.125
- value_w: bfloat16 [2, 2048, 4096], P(None, None, 'tp'), may hold values from -0.125 to 0.125
- out_w: bfloat16 [2, 8192, 2048], P(None, 'tp'), may hold values from -0.1875 to 0.1875
- head_temp: float32 [2, 16], P(None, 'tp'), may hold values from 1.5 to 8, as said below
- final_gain: bfloat16 [2048], replicated, may hold values from 0.099609375 to 1.8984375
Outputs:
- result: float32 [2048, 2048], P(('sp', 'tp'))
The draws below stay inside these ranges and needn't reach their ends.
Inputs may be any that keep to these rules, and one draw needn't show every extreme that they name: `head_temp`: a positive scale for each head's scores.
All inputs are finite; a program needn't handle non-finite values.
Results may differ from the reference program's by a relative error of at most 0.04.
Values may be sent and summed in bfloat16 or wider, within the bound.
A program may use at most 192 MiB of HBM per device.

```python
import math
import jax
import jax.numpy as jnp
from jax import lax

D = 2048
HEAD_DIM = 512
HEADS = 16
KV_HEADS = 8
SOURCE = 4096
TARGET = 2048
N_TP = 4


def draw_head_temp(key, part):
    moderate_key = jax.random.fold_in(key, 11)
    moderate = jnp.exp(jax.random.uniform(moderate_key, (2, HEADS), jnp.float32, math.log(1.5), math.log(3.5)))
    return moderate


def block_scale(stream_key, extent, cuts, smallest, high):
    level = 1.0
    for position, parts in cuts:
        draws = jax.random.uniform(jax.random.fold_in(jax.random.fold_in(stream_key, 6), position), (parts,), jnp.float32, smallest / len(cuts), high / len(cuts))
        level = level * jnp.repeat(jnp.exp(draws), extent[position] // parts).reshape((-1,) + (1,) * (len(extent) - 1 - position))
    return level


def noise(rng, extent, width, bound, cuts=(), kind=jnp.bfloat16):
    factor_of = block_scale(rng, extent, cuts, -0.22, 0.18) if cuts else 1.0
    array = jax.random.normal(rng, extent, jnp.float32) * width * factor_of
    return jnp.minimum(jnp.maximum(array, -bound), bound).astype(kind)


def setup_inputs(seed: int = 0) -> dict:
    splits = jax.random.split(jax.random.key(seed), 11)
    target = noise(splits[0], (TARGET, D), 1.0, 6.0, ((0, 32),))
    source = noise(splits[1], (SOURCE, D), 1.0, 6.0, ((0, 32),))
    target_gain = jnp.clip(1.0 + 0.18 * jax.random.normal(splits[2], (2, D), jnp.float32), 0.099609375, 1.8984375).astype(jnp.bfloat16)
    source_gain = jnp.clip(1.0 + 0.18 * jax.random.normal(splits[3], (2, D), jnp.float32), 0.099609375, 1.8984375).astype(jnp.bfloat16)
    query_w = noise(splits[4], (2, D, HEADS * HEAD_DIM), D ** -0.5, 0.125, ((2, 4),))
    key_w = noise(splits[5], (2, D, KV_HEADS * HEAD_DIM), D ** -0.5, 0.125, ((2, 4),))
    value_w = noise(splits[6], (2, D, KV_HEADS * HEAD_DIM), D ** -0.5, 0.125, ((2, 4),))
    out_w = noise(splits[7], (2, HEADS * HEAD_DIM, D), (3.0 * (HEADS * HEAD_DIM) ** -0.5), 0.1875, ((1, 4),))
    head_temp = draw_head_temp(jax.random.fold_in(splits[10], 71), 0)
    final_gain = jnp.clip(1.0 + 0.18 * jax.random.normal(splits[9], (D,), jnp.float32), 0.099609375, 1.8984375).astype(jnp.bfloat16)
    return dict(target=target, source=source, target_gain=target_gain, source_gain=source_gain, query_w=query_w, key_w=key_w, value_w=value_w, out_w=out_w, head_temp=head_temp, final_gain=final_gain)


EPS = 1e-06

def unit_rows(matrix):
    values = matrix.astype(jnp.float32)
    return values * lax.rsqrt(lax.optimization_barrier(jnp.mean(values * values, axis=-1, keepdims=True)) + EPS)

def attend_head(queries, key_rows, value_rows, scales):
    scores = jnp.dot(queries, key_rows.T, preferred_element_type=jnp.float32) * scales
    row_max = lax.optimization_barrier(jnp.max(scores, axis=-1, keepdims=True))
    exponent = jnp.exp(scores - row_max)
    row_total = lax.optimization_barrier(jnp.sum(exponent, axis=-1, keepdims=True))
    weights = exponent.astype(jnp.bfloat16)
    summed = jnp.dot(weights, value_rows, preferred_element_type=jnp.float32)
    return (summed / row_total).astype(jnp.bfloat16)

def reference(target, source, target_gain, source_gain, query_w, key_w, value_w, out_w, head_temp, final_gain):
    unit_source = unit_rows(source)
    group_size = HEADS // KV_HEADS
    head_share = HEADS // N_TP
    hidden_state = target.astype(jnp.float32)
    for layer_index in range(2):
        normed_source = (unit_source * source_gain[layer_index].astype(jnp.float32)).astype(jnp.bfloat16)
        key_rows = jnp.dot(normed_source, key_w[layer_index], preferred_element_type=jnp.float32).astype(jnp.bfloat16)
        value_rows = jnp.dot(normed_source, value_w[layer_index], preferred_element_type=jnp.float32).astype(jnp.bfloat16)
        key_rows = key_rows.reshape(SOURCE, KV_HEADS, HEAD_DIM)
        value_rows = value_rows.reshape(SOURCE, KV_HEADS, HEAD_DIM)
        normed = (unit_rows(hidden_state) * target_gain[layer_index].astype(jnp.float32)).astype(jnp.bfloat16)
        queries = jnp.dot(normed, query_w[layer_index], preferred_element_type=jnp.float32).astype(jnp.bfloat16)
        queries = queries.reshape(TARGET, HEADS, HEAD_DIM)
        scales = head_temp[layer_index].astype(jnp.float32) * HEAD_DIM ** (-0.5)

        def one_head(head_index):
            shared_head = head_index // group_size
            return attend_head(queries[:, head_index], key_rows[:, shared_head], value_rows[:, shared_head], scales[head_index])
        heads_out = lax.map(one_head, jnp.arange(HEADS, dtype=jnp.int32))
        heads_out = heads_out.reshape(N_TP, head_share, TARGET, HEAD_DIM)
        out_parts = out_w[layer_index].reshape(N_TP, head_share, HEAD_DIM, D)

        def part_term(running, inputs):
            head_block, weights = inputs
            partial_value = jnp.einsum('htd,hde->te', head_block.astype(jnp.float32), weights.astype(jnp.float32))
            rounded = lax.optimization_barrier(partial_value.astype(jnp.bfloat16))
            return (running + rounded.astype(jnp.float32), None)
        mixed, unused = lax.scan(part_term, jnp.zeros((TARGET, D), jnp.float32), (heads_out, out_parts))
        hidden_state = hidden_state + mixed
    return unit_rows(hidden_state) * final_gain.astype(jnp.float32)
```

```python
import functools
import math

import jax
import jax.numpy as jnp
from jax import lax
from jax.experimental import pallas as pl
from jax.experimental.pallas import tpu as pltpu
from jax.sharding import PartitionSpec as P

HEAD_DIM = 512
EPS = 1e-06
FLOOR = -1e30
CHUNK = 512
ROWS = 512
LOG2E = math.log2(math.e)


def unit_rows(matrix):
    values = matrix.astype(jnp.float32)
    return values * lax.rsqrt(jnp.mean(values * values, axis=-1, keepdims=True) + EPS)


def attend_kernel(rows, query_ref, source_ref, mix_ref, total_ref, top_ref, sum_ref):
    step = pl.program_id(0)
    count = query_ref.shape[0]

    @pl.when(step == 0)
    def _():
        total_ref[...] = jnp.zeros_like(total_ref)
        sum_ref[...] = jnp.zeros_like(sum_ref)
        top_ref[...] = jnp.full_like(top_ref, FLOOR)

    for start in range(0, count, rows):
        block = pl.ds(start, rows)
        scores = lax.dot_general(
            query_ref[block, :],
            source_ref[...],
            (((1,), (1,)), ((), ())),
            preferred_element_type=jnp.float32,
        )
        old_top = top_ref[block, :1]
        new_top = jnp.maximum(old_top, jnp.max(scores, axis=-1, keepdims=True))
        shrink = jnp.exp2(old_top - new_top)
        expo = jnp.exp2(scores - new_top)
        top_ref[block, :] = jnp.broadcast_to(new_top, (rows, top_ref.shape[1]))
        new_sum = sum_ref[block, :1] * shrink + jnp.sum(expo, axis=-1, keepdims=True)
        sum_ref[block, :] = jnp.broadcast_to(new_sum, (rows, sum_ref.shape[1]))
        total_ref[block, :] = total_ref[block, :] * shrink + jnp.dot(
            expo.astype(jnp.bfloat16), source_ref[...], preferred_element_type=jnp.float32
        )

    @pl.when(step == pl.num_programs(0) - 1)
    def _():
        for start in range(0, count, rows):
            block = pl.ds(start, rows)
            mix_ref[block, :] = (total_ref[block, :] / sum_ref[block, :1]).astype(mix_ref.dtype)


def attend(query, source, chunk=CHUNK, rows=ROWS):
    count, width = query.shape
    positions = source.shape[0]
    chunk = math.gcd(chunk, positions)
    rows = math.gcd(rows, count)
    return pl.pallas_call(
        functools.partial(attend_kernel, rows),
        grid=(positions // chunk,),
        out_shape=jax.ShapeDtypeStruct((count, width), jnp.bfloat16),
        in_specs=[
            pl.BlockSpec((count, width), lambda j: (0, 0), pipeline_mode=pl.Buffered(1)),
            pl.BlockSpec((chunk, width), lambda j: (j, 0)),
        ],
        out_specs=pl.BlockSpec((count, width), lambda j: (0, 0), pipeline_mode=pl.Buffered(1)),
        scratch_shapes=[
            pltpu.VMEM((count, width), jnp.float32),
            pltpu.VMEM((count, 128), jnp.float32),
            pltpu.VMEM((count, 128), jnp.float32),
        ],
        compiler_params=pltpu.CompilerParams(
            dimension_semantics=("arbitrary",), vmem_limit_bytes=56 * 1024 * 1024
        ),
        cost_estimate=pl.CostEstimate(
            flops=4 * count * positions * width,
            bytes_accessed=2 * positions * width,
            transcendentals=count * positions,
        ),
    )(query, source)


def per_device(
    target, source, target_gain, source_gain, query_w, key_w, value_w, out_w, head_temp, final_gain
):
    width = target.shape[1]
    heads = query_w.shape[2] // HEAD_DIM
    shared = key_w.shape[2] // HEAD_DIM
    group = heads // shared
    positions = lax.all_gather(
        unit_rows(source).astype(jnp.bfloat16), ("sp", "tp"), axis=0, tiled=True
    )
    hidden_state = target.astype(jnp.float32)
    for layer in range(2):
        gain = source_gain[layer].astype(jnp.float32)
        normed = (unit_rows(hidden_state) * target_gain[layer].astype(jnp.float32)).astype(
            jnp.bfloat16
        )
        queries = jnp.dot(
            lax.all_gather(normed, "tp", axis=0, tiled=True),
            query_w[layer],
            preferred_element_type=jnp.float32,
        ).astype(jnp.bfloat16)
        count = queries.shape[0]
        scales = head_temp[layer] * (HEAD_DIM ** (-0.5) * LOG2E)
        lifted = []
        for head in range(heads):
            columns = slice((head // group) * HEAD_DIM, (head // group + 1) * HEAD_DIM)
            lifted.append(
                (
                    lax.dot_general(
                        queries[:, head * HEAD_DIM : (head + 1) * HEAD_DIM],
                        key_w[layer][:, columns],
                        (((1,), (1,)), ((), ())),
                        preferred_element_type=jnp.float32,
                    )
                    * (gain * scales[head])
                ).astype(jnp.bfloat16)
            )
        mix = attend(jnp.concatenate(lifted, axis=0), positions)
        attended = []
        for head in range(heads):
            columns = slice((head // group) * HEAD_DIM, (head // group + 1) * HEAD_DIM)
            own = (mix[head * count : (head + 1) * count].astype(jnp.float32) * gain).astype(
                jnp.bfloat16
            )
            attended.append(
                jnp.dot(
                    own, value_w[layer][:, columns], preferred_element_type=jnp.float32
                ).astype(jnp.bfloat16)
            )
        mixed = lax.psum_scatter(
            jnp.dot(
                jnp.concatenate(attended, axis=1),
                out_w[layer],
                preferred_element_type=jnp.float32,
            ).astype(jnp.bfloat16),
            "tp",
            scatter_dimension=0,
            tiled=True,
        ).astype(jnp.float32)
        hidden_state = hidden_state + mixed
    return unit_rows(hidden_state) * final_gain.astype(jnp.float32)


def solution(mesh):
    in_specs = (
        P(("sp", "tp"), None),
        P(("sp", "tp"), None),
        P(),
        P(),
        P(None, None, "tp"),
        P(None, None, "tp"),
        P(None, None, "tp"),
        P(None, "tp", None),
        P(None, "tp"),
        P(),
    )
    out_specs = P(("sp", "tp"), None)
    return jax.shard_map(
        per_device, mesh=mesh, in_specs=in_specs, out_specs=out_specs, check_vma=False
    )
```
